32 devices in a mesh: ep: 4 (over y, x), tp: 8 (over z, core).
Axes of the slice: x: 2, y: 2, z: 4, core: 2. Of those that a mesh axis runs over, the one named last changes fastest.
Arguments:
- q_latent: bfloat16 [4096, 512], P('ep'), may hold values from -6 to 6
- kv_latent: bfloat16 [4096, 256], P('ep'), may hold values from -6 to 6
- rope_key: bfloat16 [4096, 32], P('ep'), may hold values from -1200 to 1200
- q_gain: float32 [512], replicated, may hold values from 0.1 to 1.9
- kv_gain: float32 [256], replicated, may hold values from 0.1 to 1.9
- w_query: bfloat16 [512, 1536], P(None, 'tp'), may hold values from -0.25 to 0.25
- w_keyval: bfloat16 [256, 2048], P(None, 'tp'), may hold values from -0.375 to 0.375
- w_output: bfloat16 [1024, 2048], P(None, 'tp'), may hold values from -0.1875 to 0.1875
- moe_input: bfloat16 [1024, 2048], P('ep'), may hold values from -6 to 6
- moe_gain: float32 [2048], replicated, may hold values from 0.1 to 1.9
- routes: int32 [1024, 2], P('ep'), may hold values from 0 to 3, all different within a row; in each aligned block of 32 rows (0 to 31, 32 to 63, ...) at most 24 rows name the same one
- route_weight: float32 [1024, 2], P('ep'), may hold values from 0.25 to 2
- expert_gate: bfloat16 [4, 2048, 4096], P('ep', None, 'tp'), may hold values from -0.125 to 0.125
- expert_up: bfloat16 [4, 2048, 4096], P('ep', None, 'tp'), may hold values from -0.125 to 0.125
- expert_down: bfloat16 [4, 4096, 2048], P('ep', 'tp'), may hold values from -0.09375 to 0.09375
- shared_gate: bfloat16 [2048, 2048], P(None, 'tp'), may hold values from -0.125 to 0.125
- shared_up: bfloat16 [2048, 2048], P(None, 'tp'), may hold values from -0.125 to 0.125
- shared_down: bfloat16 [2048, 2048], P('tp'), may hold values from -0.125 to 0.125
Outputs:
- mixed: bfloat16 [4096, 2048], P('ep', 'tp')
- moe_out: bfloat16 [1024, 2048], P(('ep', 'tp'))
The draws below stay inside these ranges and needn't reach their ends.
Inputs may be any that keep to these rules, and one draw needn't show every extreme that they name: `routes`: in each aligned block of 32 rows (the rows of one device's output) no expert is named by more than 24 rows, a bound that some block reaches. Each row names 2 different experts.
All inputs are finite; a program needn't handle non-finite values.
Results may differ from the reference program's by a relative error of at most 0.023.
Values may be sent and summed in bfloat16 or wider, within the bound.
A program may use at most 128 MiB of HBM per device.

```python
import math
import jax
import jax.numpy as jnp
import numpy as np
from jax import lax

D = 2048
HEADS = 16
NOPE = 64
ROPE_DIM = 32
VDIM = 64
QLAT = 512
KVLAT = 256
TOKA_EP = 1024
TOK_A = 4096
MOE_DEV = 32
TOK_B = 1024
EXPERTS = 4
FE = 4096
FS = 2048
FE_PART = 512
FS_PART = 256
TOP = 2
CAP = 24
N_EP = 4
N_TP = 8


def draw_rope_key(key, part):
    drawn = jax.random.normal(jax.random.fold_in(key, 11), (TOK_A, ROPE_DIM), jnp.float32)
    drawn = jnp.clip(drawn, -6.0, 6.0)
    return drawn.astype(jnp.bfloat16)


def block_scale(own_key, extent, split, smallest, top_value):
    level = 1.0
    for axis_at, parts in split:
        heights = jax.random.uniform(jax.random.fold_in(jax.random.fold_in(own_key, 6), axis_at), (parts,), jnp.float32, smallest / len(split), top_value / len(split))
        level = level * jnp.repeat(jnp.exp(heights), extent[axis_at] // parts).reshape((-1,) + (1,) * (len(extent) - 1 - axis_at))
    return level


def routed_block(own_key, own, number, rows, amount, top, bound, skew):
    order = jax.random.permutation(own_key, amount)
    packed, ordinary = shares(amount, rows * top, bound, skew, True), shares(amount, rows * top, bound, skew, False)
    places = jnp.arange(amount)

    def named(lengths, offset_by):
        used = int((lengths > 0).sum())
        fixed = max(1, used // 4)
        passed = fixed + (places - fixed + offset_by * (used - fixed)) % max(1, amount - fixed)
        return jnp.zeros((amount,), jnp.int32).at[order[jnp.where(places < fixed, places, passed)]].set(jnp.asarray(lengths, jnp.int32))

    lengths = jnp.where(number % 4 == 0, named(packed, number // 4), named(ordinary, number - number // 4 - 1))
    mixed = jax.random.permutation(jax.random.fold_in(own, 3), amount)
    source_of, taker = mixed[0:amount // 2 * 2:2], mixed[1:amount // 2 * 2:2]
    room = jnp.minimum(lengths[source_of] - 1, bound - lengths[taker]) // 2
    room = jnp.where((source_of == order[0]) | (taker == order[0]) | (lengths[taker] == 0), 0, jnp.maximum(room, 0))
    passed = jax.random.randint(jax.random.fold_in(own, 4), (amount // 2,), 0, 1 << 20) % (room + 1)
    lengths = lengths.at[source_of].add(-passed).at[taker].add(passed)
    members = jnp.searchsorted(jnp.cumsum(lengths), jnp.arange(rows * top), side="right").astype(jnp.int32)
    grid = members.reshape(top, rows).T
    grid = grid[jax.random.permutation(jax.random.fold_in(own, 1), rows)]
    offset_by = jax.random.randint(jax.random.fold_in(own, 2), (rows, 1), 0, top)
    return jnp.take_along_axis(grid, (jnp.arange(top)[None, :] + offset_by) % top, axis=1)


def shares(amount, total, bound, slope, full):
    portions = [(1 << 20) // math.isqrt(rank ** slope) + 1 for rank in range(1, amount + 1)]
    largest = bound if full else min(bound, max(-(-total // amount), total * portions[0] // sum(portions)))
    least = 1 if total - largest >= amount - 1 else 0
    holding, rest = [largest] + [least] * (amount - 1), total - largest - least * (amount - 1)
    while rest > 0:
        free = [i for i in range(1, amount) if holding[i] < largest] or [i for i in range(1, amount) if holding[i] < bound]
        whole, left = sum([portions[i] for i in free]), rest
        for i in free:
            extra = min(bound - holding[i], max(1, left * portions[i] // whole), rest)
            holding[i] = holding[i] + extra
            rest = rest - extra
    return np.array(holding)


def bell_draw(key, shape, deviation, bound, pieces=(), held_as=jnp.bfloat16):
    values = jax.random.normal(key, shape, jnp.float32) * deviation
    if len(pieces) > 0:
        values = block_scale(key, shape, pieces, -0.22, 0.18) * values
    return jnp.clip(values, min=-bound, max=bound).astype(held_as)


def setup_inputs(seed: int = 0) -> dict:
    streams_of = jax.random.split(jax.random.key(seed), 19)
    q_latent = bell_draw(streams_of[0], (TOK_A, QLAT), 1.0, 6.0, ((0, 4),))
    kv_latent = bell_draw(streams_of[1], (TOK_A, KVLAT), 1.0, 6.0, ((0, 4),))
    rope_key = draw_rope_key(jax.random.fold_in(streams_of[18], 71), 0)
    q_gain = jnp.clip(1.0 + 0.18 * jax.random.normal(streams_of[3], (QLAT,), jnp.float32), 0.1, 1.9)
    kv_gain = jnp.clip(1.0 + 0.18 * jax.random.normal(streams_of[4], (KVLAT,), jnp.float32), 0.1, 1.9)
    w_query = bell_draw(streams_of[5], (QLAT, HEADS * (NOPE + ROPE_DIM)), QLAT ** -0.5, 0.25, ((1, 8),))
    w_keyval = bell_draw(streams_of[6], (KVLAT, HEADS * (NOPE + VDIM)), KVLAT ** -0.5, 0.375, ((1, 8),))
    w_output = bell_draw(streams_of[7], (HEADS * VDIM, D), (HEADS * VDIM) ** -0.5, 0.1875, ((1, 8),))
    moe_input = bell_draw(streams_of[8], (TOK_B, D), 1.0, 6.0, ((0, 4),))
    moe_gain = jnp.clip(1.0 + 0.18 * jax.random.normal(streams_of[9], (D,), jnp.float32), 0.1, 1.9)
    routes_keys = jax.random.split(jax.random.fold_in(streams_of[10], 1), TOK_B // MOE_DEV)
    routes_turns = jax.random.permutation(jax.random.fold_in(streams_of[10], 3), TOK_B // MOE_DEV)
    routes = jax.vmap(lambda own, number: routed_block(jax.random.fold_in(streams_of[10], 2), own, number, MOE_DEV, EXPERTS, TOP, CAP, 1))(routes_keys, routes_turns).reshape((TOK_B, TOP))
    route_weight = jnp.clip(0.25 + 1.75 * jax.random.uniform(streams_of[11], (TOK_B, TOP), jnp.float32) ** block_scale(streams_of[11], (TOK_B, TOP), ((0, 4),), -0.2, 0.2), 0.25, 2.0)
    expert_gate = bell_draw(streams_of[12], (EXPERTS, D, FE), D ** -0.5, 0.125, ((0, 4), (2, 8)))
    expert_up = bell_draw(streams_of[13], (EXPERTS, D, FE), D ** -0.5, 0.125, ((0, 4), (2, 8)))
    expert_down = bell_draw(streams_of[14], (EXPERTS, FE, D), FE ** -0.5, 0.09375, ((0, 4), (1, 8)))
    shared_gate = bell_draw(streams_of[15], (D, FS), D ** -0.5, 0.125, ((1, 8),))
    shared_up = bell_draw(streams_of[16], (D, FS), D ** -0.5, 0.125, ((1, 8),))
    shared_down = bell_draw(streams_of[17], (FS, D), FS ** -0.5, 0.125, ((0, 8),))
    return dict(q_latent=q_latent, kv_latent=kv_latent, rope_key=rope_key, q_gain=q_gain, kv_gain=kv_gain, w_query=w_query, w_keyval=w_keyval, w_output=w_output, moe_input=moe_input, moe_gain=moe_gain, routes=routes, route_weight=route_weight, expert_gate=expert_gate, expert_up=expert_up, expert_down=expert_down, shared_gate=shared_gate, shared_up=shared_up, shared_down=shared_down)


norm_eps = 1e-06
layer_eps = 1e-05
rotary_base = 10000.0
floor_value = -1e+30

def rms_scale(values, gain):
    widened = values.astype(jnp.float32)
    return (widened * lax.rsqrt(lax.optimization_barrier(jnp.mean(widened * widened, -1, keepdims=True)) + norm_eps) * gain).astype(jnp.bfloat16)

def layer_scale(values, gain):
    widened = values.astype(jnp.float32)
    centred = widened - lax.optimization_barrier(jnp.mean(widened, -1, keepdims=True))
    return (centred * lax.rsqrt(lax.optimization_barrier(jnp.mean(centred * centred, -1, keepdims=True)) + layer_eps) * gain).astype(jnp.bfloat16)

def rotary_tables(positions):
    halfway = ROPE_DIM // 2
    inverse = rotary_base ** (-(jnp.arange(halfway, dtype=jnp.float32) * 2.0 / ROPE_DIM))
    angles = positions.astype(jnp.float32)[:, None] * inverse[None, :]
    return (jnp.cos(angles), jnp.sin(angles))

def rotate(values, cosine_table, sine_table):
    halfway = values.shape[-1] // 2
    first_half = values[..., :halfway]
    second_half = values[..., halfway:]
    return jnp.concatenate([first_half * cosine_table - second_half * sine_table, second_half * cosine_table + first_half * sine_table], -1)

def merge_block(carried, stats):
    running_max, running_sum, running_acc = carried
    block_max, block_sum, attended = stats
    new_max = jnp.maximum(running_max, block_max)
    old_weight = jnp.exp(running_max - new_max)
    new_weight = jnp.exp(block_max - new_max)
    return (new_max, running_sum * old_weight + block_sum * new_weight, running_acc * old_weight[..., None] + attended.astype(jnp.float32) * new_weight[..., None])

def group_sum(hidden, down_weight, group_width):

    def add_group(group_index, total):
        hidden_cols = lax.dynamic_slice_in_dim(hidden, group_index * group_width, group_width, 1)
        weight_rows = lax.dynamic_slice_in_dim(down_weight, group_index * group_width, group_width, 0)
        product = jnp.dot(hidden_cols, weight_rows, preferred_element_type=jnp.float32)
        return total + lax.optimization_barrier(product.astype(jnp.bfloat16)).astype(jnp.float32)
    return lax.fori_loop(0, N_TP, add_group, jnp.zeros((hidden.shape[0], down_weight.shape[1]), jnp.float32))

def reference(q_latent, kv_latent, rope_key, q_gain, kv_gain, w_query, w_keyval, w_output, moe_input, moe_gain, routes, route_weight, expert_gate, expert_up, expert_down, shared_gate, shared_up, shared_down):
    positions = jnp.arange(TOK_A, dtype=jnp.int32)
    cosine_table, sine_table = rotary_tables(positions)
    q_normed = rms_scale(q_latent, q_gain)
    kv_normed = rms_scale(kv_latent, kv_gain)
    key_rot = rotate(rope_key.astype(jnp.float32), cosine_table, sine_table).astype(jnp.bfloat16)
    projected = jnp.dot(q_normed, w_query, preferred_element_type=jnp.float32).reshape(TOK_A, HEADS, NOPE + ROPE_DIM)
    queries = jnp.concatenate([projected[..., :NOPE], rotate(projected[..., NOPE:], cosine_table[:, None, :], sine_table[:, None, :])], -1).astype(jnp.bfloat16)
    keyvals = jnp.dot(kv_normed, w_keyval, preferred_element_type=jnp.float32).astype(jnp.bfloat16)
    keyvals = keyvals.reshape(TOK_A, HEADS, NOPE + VDIM)
    scale = float(NOPE + ROPE_DIM) ** (-0.5)

    def visit_group(group_index):
        first_row = group_index * TOKA_EP
        query_block = lax.dynamic_slice_in_dim(queries, first_row, TOKA_EP, 0).astype(jnp.float32)
        query_pos = first_row + jnp.arange(TOKA_EP, dtype=jnp.int32)

        def visit_block(block_index, carried):
            key_first = block_index * TOKA_EP
            keyval_block = lax.dynamic_slice_in_dim(keyvals, key_first, TOKA_EP, 0).astype(jnp.float32)
            rotated_block = lax.dynamic_slice_in_dim(key_rot, key_first, TOKA_EP, 0).astype(jnp.float32)
            key_pos = key_first + jnp.arange(TOKA_EP, dtype=jnp.int32)
            scores = jnp.einsum('qhd,khd->hqk', query_block[..., :NOPE], keyval_block[..., :NOPE])
            scores = (scores + jnp.einsum('qhd,kd->hqk', query_block[..., NOPE:], rotated_block)) * scale
            allowed = key_pos[None, :] <= query_pos[:, None]
            scores = jnp.where(allowed[None], scores, -jnp.inf)
            block_max = lax.optimization_barrier(jnp.max(scores, -1))
            weights = jnp.exp(scores - block_max[..., None])
            block_sum = lax.optimization_barrier(jnp.sum(weights, -1))
            rounded = lax.optimization_barrier(weights.astype(jnp.bfloat16)).astype(jnp.float32)
            attended = jnp.einsum('hqk,khd->qhd', rounded, keyval_block[..., NOPE:])
            attended = lax.optimization_barrier(attended.astype(jnp.bfloat16)).astype(jnp.float32)
            return merge_block(carried, (block_max.T, block_sum.T, attended))
        initial = (jnp.full((TOKA_EP, HEADS), floor_value, jnp.float32), jnp.zeros((TOKA_EP, HEADS), jnp.float32), jnp.zeros((TOKA_EP, HEADS, VDIM), jnp.float32))
        running_max, running_sum, running_acc = lax.fori_loop(0, group_index + 1, visit_block, initial)
        return (running_acc / running_sum[..., None]).astype(jnp.bfloat16).reshape(TOKA_EP, HEADS * VDIM)
    heads_out = lax.map(visit_group, jnp.arange(N_EP, dtype=jnp.int32)).reshape(TOK_A, HEADS * VDIM)
    mixed = jnp.dot(heads_out, w_output, preferred_element_type=jnp.float32).astype(jnp.bfloat16)
    block_total = TOK_B // MOE_DEV
    normed = layer_scale(moe_input, moe_gain)
    entries = routes.reshape(block_total, MOE_DEV * TOP)
    onehot = (entries[..., None] == jnp.arange(EXPERTS, dtype=jnp.int32)).astype(jnp.int32)
    earlier = jnp.cumsum(onehot, 1) - onehot
    rank_in = lax.optimization_barrier(jnp.sum(earlier * onehot, -1))
    block_ids = jnp.broadcast_to(jnp.arange(block_total, dtype=jnp.int32)[:, None], entries.shape)
    token_ids = (jnp.arange(TOK_B * TOP, dtype=jnp.int32) // TOP).reshape(block_total, MOE_DEV * TOP)
    table = jnp.full((EXPERTS, block_total, CAP), -1, jnp.int32).at[entries, block_ids, rank_in].set(token_ids)

    def run_expert(operands):
        slot_token, gate_weight, up_weight, down_weight = operands
        inputs = jnp.where((slot_token >= 0)[:, None], normed[jnp.maximum(slot_token, 0)], jnp.zeros((), jnp.bfloat16))
        hidden = jax.nn.silu(jnp.dot(inputs, gate_weight, preferred_element_type=jnp.float32))
        hidden = (hidden * jnp.dot(inputs, up_weight, preferred_element_type=jnp.float32)).astype(jnp.bfloat16)
        return group_sum(hidden, down_weight, FE_PART)
    expert_sums = lax.map(run_expert, (table.reshape(EXPERTS, block_total * CAP), expert_gate, expert_up, expert_down))
    slot_of = ((entries * block_total + block_ids) * CAP + rank_in).reshape(TOK_B, TOP)
    picked = expert_sums.reshape(EXPERTS * block_total * CAP, D)[slot_of]
    routed = lax.optimization_barrier(jnp.sum(route_weight[..., None] * picked, 1))
    shared_hidden = jax.nn.silu(jnp.dot(normed, shared_gate, preferred_element_type=jnp.float32))
    shared_hidden = (shared_hidden * jnp.dot(normed, shared_up, preferred_element_type=jnp.float32)).astype(jnp.bfloat16)
    shared_total = group_sum(shared_hidden, shared_down, FS_PART)
    moe_out = (routed + shared_total).astype(jnp.bfloat16)
    return (mixed, moe_out)
```

```python
import jax
import jax.numpy as jnp
from jax import lax
from jax.experimental import pallas as pl
from jax.experimental.pallas import tpu as pltpu
from jax.sharding import PartitionSpec as P


NOPE = 64
ROPE_DIM = 32
VDIM = 64
MOE_DEV = 32


norm_eps = 1e-06
layer_eps = 1e-05
rotary_base = 10000.0
floor_value = -1e30


def rms_scale(values, gain):
    widened = values.astype(jnp.float32)
    return (
        widened * lax.rsqrt(jnp.mean(widened * widened, -1, keepdims=True) + norm_eps) * gain
    ).astype(jnp.bfloat16)


def layer_scale(values, gain):
    widened = values.astype(jnp.float32)
    centred = widened - jnp.mean(widened, -1, keepdims=True)
    return (
        centred * lax.rsqrt(jnp.mean(centred * centred, -1, keepdims=True) + layer_eps) * gain
    ).astype(jnp.bfloat16)


def rotary_tables(positions):
    halfway = ROPE_DIM // 2
    inverse = rotary_base ** (-(jnp.arange(halfway, dtype=jnp.float32) * 2.0 / ROPE_DIM))
    angles = positions.astype(jnp.float32)[:, None] * inverse[None, :]
    return (jnp.cos(angles), jnp.sin(angles))


def rotate(values, cosine_table, sine_table):
    halfway = values.shape[-1] // 2
    first_half = values[..., :halfway]
    second_half = values[..., halfway:]
    return jnp.concatenate(
        [
            first_half * cosine_table - second_half * sine_table,
            second_half * cosine_table + first_half * sine_table,
        ],
        -1,
    )


def block_stats(query_block, query_pos, keyvals, rotated_keys, key_pos):
    scale = float(NOPE + ROPE_DIM) ** (-0.5)
    scores = jnp.einsum(
        "qhd,khd->hqk",
        query_block[..., :NOPE],
        keyvals[..., :NOPE],
        preferred_element_type=jnp.float32,
    )
    scores = (
        scores
        + jnp.einsum(
            "qhd,kd->hqk", query_block[..., NOPE:], rotated_keys, preferred_element_type=jnp.float32
        )
    ) * scale
    allowed = key_pos[None, :] <= query_pos[:, None]
    scores = jnp.where(allowed[None], scores, -jnp.inf)
    block_max = jnp.max(scores, -1)
    weights = jnp.exp(scores - block_max[..., None])
    block_sum = jnp.sum(weights, -1)
    attended = jnp.einsum(
        "hqk,khd->qhd",
        weights.astype(jnp.bfloat16),
        keyvals[..., NOPE:],
        preferred_element_type=jnp.float32,
    ).astype(jnp.bfloat16)
    return (block_max.T, block_sum.T, attended)


def merge_block(carried, stats):
    running_max, running_sum, running_acc = carried
    block_max, block_sum, attended = stats
    new_max = jnp.maximum(running_max, block_max)
    old_weight = jnp.exp(running_max - new_max)
    new_weight = jnp.exp(block_max - new_max)
    return (
        new_max,
        running_sum * old_weight + block_sum * new_weight,
        running_acc * old_weight[..., None] + attended.astype(jnp.float32) * new_weight[..., None],
    )


def body(
    q_latent,
    kv_latent,
    rope_key,
    q_gain,
    kv_gain,
    w_query,
    w_keyval,
    w_output,
    moe_input,
    moe_gain,
    routes,
    route_weight,
    expert_gate,
    expert_up,
    expert_down,
    shared_gate,
    shared_up,
    shared_down,
):
    row_count = q_latent.shape[0]
    own_index = lax.axis_index("ep")
    ep_count = lax.axis_size("ep")
    tp_count = lax.axis_size("tp")
    positions = own_index * row_count + jnp.arange(row_count, dtype=jnp.int32)
    cosine_table, sine_table = rotary_tables(positions)
    q_normed = rms_scale(q_latent, q_gain)
    kv_normed = rms_scale(kv_latent, kv_gain)
    key_rotated = rotate(rope_key.astype(jnp.float32), cosine_table, sine_table).astype(
        jnp.bfloat16
    )
    heads_local = w_query.shape[1] // (NOPE + ROPE_DIM)
    projected = jnp.dot(q_normed, w_query, preferred_element_type=jnp.float32)
    projected = projected.reshape(row_count, heads_local, NOPE + ROPE_DIM)
    queries = jnp.concatenate(
        [
            projected[..., :NOPE],
            rotate(projected[..., NOPE:], cosine_table[:, None, :], sine_table[:, None, :]),
        ],
        -1,
    ).astype(jnp.bfloat16)

    def expand_keys(latent_rows):
        expanded = jnp.dot(latent_rows, w_keyval, preferred_element_type=jnp.float32).astype(
            jnp.bfloat16
        )
        return expanded.reshape(latent_rows.shape[0], heads_local, NOPE + VDIM)

    initial = (
        jnp.full((row_count, heads_local), floor_value, jnp.float32),
        jnp.zeros((row_count, heads_local), jnp.float32),
        jnp.zeros((row_count, heads_local, VDIM), jnp.float32),
    )
    carried = initial
    latent_piece = lax.all_gather(kv_normed, "ep", axis=0, tiled=True)
    rotated_piece = lax.all_gather(key_rotated, "ep", axis=0, tiled=True)
    block_count = latent_piece.shape[0] // row_count

    def visit_block(inner, offset):

        def live(current):
            latent_rows = lax.dynamic_slice_in_dim(latent_piece, offset * row_count, row_count, 0)
            rotated_rows = lax.dynamic_slice_in_dim(rotated_piece, offset * row_count, row_count, 0)
            key_pos = offset * row_count + jnp.arange(row_count, dtype=jnp.int32)
            stats = block_stats(queries, positions, expand_keys(latent_rows), rotated_rows, key_pos)
            return merge_block(current, stats)

        def skipped(current):
            return current

        return (lax.cond(offset <= own_index, live, skipped, inner), None)

    carried, unused = lax.scan(visit_block, carried, jnp.arange(block_count, dtype=jnp.int32))
    running_max, running_sum, running_acc = carried
    heads_out = (
        (running_acc / running_sum[..., None])
        .astype(jnp.bfloat16)
        .reshape(row_count, heads_local * VDIM)
    )
    mixed = jnp.dot(
        lax.all_gather(heads_out, "tp", axis=1, tiled=True),
        w_output,
        preferred_element_type=jnp.float32,
    )
    mixed = mixed.astype(jnp.bfloat16)
    width = moe_input.shape[1]
    top_count = routes.shape[1]
    local_experts = expert_gate.shape[0]
    expert_count = local_experts * ep_count
    capacity = max(2, 3 * MOE_DEV * top_count // (2 * expert_count))
    normed = layer_scale(moe_input, moe_gain)
    entries = routes.reshape(tp_count, MOE_DEV * top_count)
    onehot = (entries[..., None] == jnp.arange(expert_count, dtype=jnp.int32)).astype(jnp.int32)
    earlier = jnp.cumsum(onehot, 1) - onehot
    rank_in = jnp.sum(earlier * onehot, -1)
    block_ids = jnp.arange(tp_count, dtype=jnp.int32)[:, None]
    slot_of = ((entries * tp_count + block_ids) * capacity + rank_in).reshape(-1, top_count)
    token_ids = jnp.arange(tp_count * MOE_DEV * top_count, dtype=jnp.int32) // top_count
    slot_token = (
        jnp.full((expert_count * tp_count * capacity,), -1, jnp.int32)
        .at[slot_of.reshape(-1)]
        .set(token_ids)
    )
    outgoing = jnp.where(
        (slot_token >= 0)[:, None], normed[jnp.maximum(slot_token, 0)], jnp.zeros((), jnp.bfloat16)
    )
    outgoing = outgoing.reshape(ep_count, local_experts, tp_count, capacity, width)
    arrived = lax.all_to_all(outgoing, "ep", split_axis=0, concat_axis=0, tiled=True)
    slot_rows = arrived.shape[3]
    inputs = arrived[:, 0].reshape(-1, width)
    hidden = jax.nn.silu(jnp.dot(inputs, expert_gate[0], preferred_element_type=jnp.float32))
    hidden = (hidden * jnp.dot(inputs, expert_up[0], preferred_element_type=jnp.float32)).astype(
        jnp.bfloat16
    )
    output = jnp.dot(hidden, expert_down[0], preferred_element_type=jnp.float32)
    results = [output.astype(jnp.bfloat16).reshape(ep_count, tp_count, slot_rows, width)]
    partial_value = jnp.stack(results, 1)
    shared_hidden = jax.nn.silu(jnp.dot(normed, shared_gate, preferred_element_type=jnp.float32))
    shared_hidden = (
        shared_hidden * jnp.dot(normed, shared_up, preferred_element_type=jnp.float32)
    ).astype(jnp.bfloat16)
    shared_part = jnp.dot(shared_hidden, shared_down, preferred_element_type=jnp.float32).astype(
        jnp.bfloat16
    )
    slot_total, shared_total = (
        lax.psum_scatter(
            partial_value.astype(jnp.float32).astype(jnp.bfloat16),
            "tp",
            scatter_dimension=2,
            tiled=True,
        ).astype(jnp.float32),
        lax.psum_scatter(
            shared_part.astype(jnp.float32)
            .reshape(1, 1, tp_count, MOE_DEV, width)
            .astype(jnp.bfloat16),
            "tp",
            scatter_dimension=2,
            tiled=True,
        ).astype(jnp.float32),
    )
    arrived_sums = lax.all_to_all(
        slot_total.astype(jnp.bfloat16), "ep", split_axis=0, concat_axis=0, tiled=True
    ).astype(slot_total.dtype)
    own_block = lax.axis_index("tp")
    own_entries = lax.dynamic_slice_in_dim(routes, own_block * MOE_DEV, MOE_DEV, 0)
    own_rank = lax.dynamic_slice_in_dim(
        rank_in.reshape(-1, top_count), own_block * MOE_DEV, MOE_DEV, 0
    )
    own_weight = lax.dynamic_slice_in_dim(route_weight, own_block * MOE_DEV, MOE_DEV, 0)
    picked = arrived_sums.reshape(-1, width)[own_entries * capacity + own_rank]
    moe_out = (
        jnp.sum(own_weight[..., None] * picked, 1) + shared_total.reshape(MOE_DEV, width)
    ).astype(jnp.bfloat16)
    return (mixed, moe_out)


def move(value, ep_flip, tp_flip):
    ep_count = lax.axis_size("ep")
    tp_count = lax.axis_size("tp")
    pairs = [
        (e * tp_count + t, (e ^ ep_flip) * tp_count + (t ^ tp_flip))
        for e in range(ep_count)
        for t in range(tp_count)
    ]
    return lax.ppermute(value, ("ep", "tp"), pairs)


def attention_kernel(heads, half, scale, ep_ref, q_ref, k_ref, v_ref, out_ref):
    own = ep_ref[0]
    blocks = ep_ref[1]
    index = pl.program_id(0)
    rows = q_ref.shape[1]
    factor = scale * 1.4426950408889634
    local = 2 * half

    def attend(carry, query, head, start, width, masked):
        old_max, acc = carry
        keys = k_ref[head, pl.ds(start, width), :]
        values = v_ref[head, pl.ds(start, width), :]
        scores = lax.dot_general(
            query, keys, (((1,), (1,)), ((), ())), preferred_element_type=jnp.float32
        )
        if masked:
            row = lax.broadcasted_iota(jnp.int32, scores.shape, 0)
            column = lax.broadcasted_iota(jnp.int32, scores.shape, 1)
            scores = jnp.where(column <= row, scores, -jnp.inf)
        new_max = jnp.maximum(old_max, jnp.max(scores, -1, keepdims=True))
        weights = jnp.exp2((scores - new_max) * factor).astype(jnp.bfloat16)
        product = jnp.dot(weights, values, preferred_element_type=jnp.float32)
        acc = acc * jnp.exp2((old_max - new_max) * factor) + product
        return new_max, acc

    outs = []
    for head in range(heads):
        query = q_ref[head]
        carry = (
            jnp.full((rows, 1), floor_value, jnp.float32),
            jnp.zeros((rows, v_ref.shape[2]), jnp.float32),
        )
        carry = attend(carry, query, head, pl.multiple_of(index * rows, rows), rows, True)
        carry = lax.fori_loop(
            0,
            index,
            lambda i, c: attend(c, query, head, pl.multiple_of(i * rows, rows), rows, False),
            carry,
        )

        def remote(source, c):
            slot = lax.bitwise_xor(own, source) - 1
            for part in range(2):
                start = local + (part * (blocks - 1) + slot) * half
                c = attend(c, query, head, pl.multiple_of(start, half), half, False)
            return c

        carry = lax.fori_loop(0, own, remote, carry)
        acc = carry[1]
        outs.append(acc[:, :VDIM] / acc[:, VDIM : VDIM + 1])
    out_ref[...] = jnp.concatenate(outs, -1).astype(jnp.bfloat16)


def flash(own_index, ep_count, queries, keys, values):
    heads, row_count, width = queries.shape
    tile = min(256, row_count)
    total = keys.shape[1]
    scale = float(NOPE + ROPE_DIM) ** (-0.5)
    return pl.pallas_call(
        lambda *refs: attention_kernel(heads, row_count // 2, scale, *refs),
        out_shape=jax.ShapeDtypeStruct((row_count, heads * VDIM), jnp.bfloat16),
        grid_spec=pltpu.PrefetchScalarGridSpec(
            num_scalar_prefetch=1,
            grid=(row_count // tile,),
            in_specs=[
                pl.BlockSpec((heads, tile, width), lambda i, s: (0, i, 0)),
                pl.BlockSpec((heads, total, width), lambda i, s: (0, 0, 0)),
                pl.BlockSpec((heads, total, width), lambda i, s: (0, 0, 0)),
            ],
            out_specs=pl.BlockSpec((tile, heads * VDIM), lambda i, s: (i, 0)),
        ),
        cost_estimate=pl.CostEstimate(
            flops=2 * heads * row_count * total * width * 2,
            bytes_accessed=4 * heads * total * width,
            transcendentals=heads * row_count * total,
        ),
        compiler_params=pltpu.CompilerParams(vmem_limit_bytes=48 * 1024 * 1024),
        name="attend",
    )(jnp.stack([own_index, jnp.int32(ep_count)]).astype(jnp.int32), queries, keys, values)


def dense_body(
    q_latent,
    kv_latent,
    rope_key,
    q_gain,
    kv_gain,
    w_query,
    w_keyval,
    w_output,
    moe_input,
    moe_gain,
    routes,
    route_weight,
    expert_gate,
    expert_up,
    expert_down,
    shared_gate,
    shared_up,
    shared_down,
):
    row_count = q_latent.shape[0]
    half = row_count // 2
    own = lax.axis_index("ep")
    ep_count = lax.axis_size("ep")
    tp_count = lax.axis_size("tp")
    tp_index = lax.axis_index("tp")
    core = tp_index % 2
    depth = tp_index // 2
    depth_count = tp_count // 2
    positions = own * row_count + jnp.arange(row_count, dtype=jnp.int32)
    cosine_table, sine_table = rotary_tables(positions)
    latent = kv_latent.shape[1]
    width = moe_input.shape[1]

    kv_normed = rms_scale(kv_latent, kv_gain)
    key_rotated = rotate(rope_key.astype(jnp.float32), cosine_table, sine_table).astype(
        jnp.bfloat16
    )
    packed = jnp.concatenate(
        [
            lax.dynamic_slice_in_dim(kv_normed, core * half, half, 0),
            lax.dynamic_slice_in_dim(key_rotated, core * half, half, 0).reshape(-1, latent),
        ],
        0,
    )
    packs = [move(packed, k, 0) for k in range(1, ep_count)]
    packs_mine = jnp.stack(packs)
    packs_other = move(packs_mine, 0, 1)

    grouped = moe_input.reshape(depth_count, 2, MOE_DEV, width)
    own_rows = layer_scale(
        lax.dynamic_index_in_dim(grouped, core, 1, keepdims=False).reshape(-1, width), moe_gain
    )
    other_rows = layer_scale(
        lax.dynamic_index_in_dim(grouped, 1 - core, 1, keepdims=False).reshape(-1, width), moe_gain
    )
    block_rows = own_rows.shape[0]
    arrived = [move(own_rows, k, 0) for k in range(1, ep_count)]
    rows_mine = jnp.concatenate([own_rows] + arrived, 0)
    rows_other = move(rows_mine, 0, 1)

    heads_local = w_query.shape[1] // (NOPE + ROPE_DIM)
    q_normed = rms_scale(q_latent, q_gain)
    projected = jnp.dot(q_normed, w_query, preferred_element_type=jnp.float32)
    projected = projected.reshape(row_count, heads_local, NOPE + ROPE_DIM)
    lanes = 128
    queries = jnp.concatenate(
        [
            projected[..., :NOPE],
            rotate(projected[..., NOPE:], cosine_table[:, None, :], sine_table[:, None, :]),
            jnp.zeros((row_count, heads_local, lanes - NOPE - ROPE_DIM), jnp.float32),
        ],
        -1,
    ).astype(jnp.bfloat16)
    queries = queries.transpose(1, 0, 2)

    latents = jnp.concatenate(
        [kv_normed, packs_mine[:, :half].reshape(-1, latent), packs_other[:, :half].reshape(-1, latent)],
        0,
    )
    rotated = jnp.concatenate(
        [
            key_rotated,
            packs_mine[:, half:].reshape(-1, ROPE_DIM),
            packs_other[:, half:].reshape(-1, ROPE_DIM),
        ],
        0,
    )
    total = latents.shape[0]
    keyvals = jnp.dot(latents, w_keyval, preferred_element_type=jnp.float32).astype(jnp.bfloat16)
    keyvals = keyvals.reshape(total, heads_local, NOPE + VDIM).transpose(1, 0, 2)
    keys = jnp.concatenate(
        [
            keyvals[..., :NOPE],
            jnp.broadcast_to(rotated[None], (heads_local, total, ROPE_DIM)),
            jnp.zeros((heads_local, total, lanes - NOPE - ROPE_DIM), jnp.bfloat16),
        ],
        -1,
    )
    values = jnp.concatenate(
        [keyvals[..., NOPE:], jnp.ones((heads_local, total, lanes - VDIM), jnp.bfloat16)], -1
    )
    heads_out = flash(own, ep_count, queries, keys, values)

    head_parts = [heads_out] + [move(heads_out, 0, 2 * k) for k in range(1, depth_count)]
    heads_mine = jnp.concatenate(head_parts, 1)
    heads_other = move(heads_mine, 0, 1)
    head_rows = heads_local * VDIM

    def output_rows(side):
        return jnp.concatenate(
            [
                lax.dynamic_slice_in_dim(
                    w_output, (2 * jnp.bitwise_xor(depth, k) + side) * head_rows, head_rows, 0
                )
                for k in range(depth_count)
            ],
            0,
        )

    mixed = (
        jnp.dot(heads_mine, output_rows(core), preferred_element_type=jnp.float32)
        + jnp.dot(heads_other, output_rows(1 - core), preferred_element_type=jnp.float32)
    ).astype(jnp.bfloat16)

    def gated(inputs, gate, up, down):
        hidden = jax.nn.silu(jnp.dot(inputs, gate, preferred_element_type=jnp.float32))
        hidden = (hidden * jnp.dot(inputs, up, preferred_element_type=jnp.float32)).astype(
            jnp.bfloat16
        )
        return jnp.dot(hidden, down, preferred_element_type=jnp.float32).astype(jnp.bfloat16)

    shared_both = gated(
        jnp.concatenate([own_rows, other_rows], 0), shared_gate, shared_up, shared_down
    )
    shared_swapped = move(shared_both[block_rows:], 0, 1)
    routed_other = gated(rows_other, expert_gate[0], expert_up[0], expert_down[0])
    routed_swapped = move(routed_other, 0, 1)
    routed_mine = gated(rows_mine, expert_gate[0], expert_up[0], expert_down[0])
    pair_sum = (routed_mine.astype(jnp.float32) + routed_swapped.astype(jnp.float32)).astype(
        jnp.bfloat16
    )
    pair_sum = pair_sum.reshape(ep_count, block_rows, width)
    returned = [pair_sum[0]] + [move(pair_sum[k], k, 0) for k in range(1, ep_count)]
    own_routes = lax.dynamic_index_in_dim(
        routes.reshape(depth_count, 2, MOE_DEV, -1), core, 1, keepdims=False
    ).reshape(block_rows, -1)
    own_weight = lax.dynamic_index_in_dim(
        route_weight.reshape(depth_count, 2, MOE_DEV, -1), core, 1, keepdims=False
    ).reshape(block_rows, -1)
    summed = shared_both[:block_rows].astype(jnp.float32) + shared_swapped.astype(jnp.float32)
    for k in range(ep_count):
        weight = jnp.sum(
            jnp.where(own_routes == jnp.bitwise_xor(own, k), own_weight, 0.0), -1, keepdims=True
        )
        summed = summed + weight * returned[k].astype(jnp.float32)
    summed = summed.astype(jnp.bfloat16).reshape(depth_count, MOE_DEV, width)
    moe_out = lax.dynamic_index_in_dim(summed, depth, 0, keepdims=False).astype(jnp.float32)
    for k in range(1, depth_count):
        part = lax.dynamic_index_in_dim(summed, jnp.bitwise_xor(depth, k), 0, keepdims=False)
        moe_out = moe_out + move(part, 0, 2 * k).astype(jnp.float32)
    return (mixed, moe_out.astype(jnp.bfloat16))


def solution(mesh):
    in_specs = (
        P("ep", None),
        P("ep", None),
        P("ep", None),
        P(),
        P(),
        P(None, "tp"),
        P(None, "tp"),
        P(None, "tp"),
        P("ep", None),
        P(),
        P("ep", None),
        P("ep", None),
        P("ep", None, "tp"),
        P("ep", None, "tp"),
        P("ep", "tp", None),
        P(None, "tp"),
        P(None, "tp"),
        P("tp", None),
    )
    out_specs = (P("ep", "tp"), P(("ep", "tp"), None))
    dense = mesh.shape["ep"] <= 4
    return jax.shard_map(dense_body if dense else body, mesh=mesh, in_specs=in_specs, out_specs=out_specs, check_vma=False)
```

```python
import jax
import jax.numpy as jnp
import numpy as np
from jax import lax
from jax.experimental import pallas as pl
from jax.experimental.pallas import tpu as pltpu
from jax.sharding import PartitionSpec as P


NOPE = 64
ROPE_DIM = 32
VDIM = 64
MOE_DEV = 32


norm_eps = 1e-06
layer_eps = 1e-05
rotary_base = 10000.0
floor_value = -1e30


def rms_scale(values, gain):
    widened = values.astype(jnp.float32)
    return (
        widened * lax.rsqrt(jnp.mean(widened * widened, -1, keepdims=True) + norm_eps) * gain
    ).astype(jnp.bfloat16)


def layer_scale(values, gain):
    widened = values.astype(jnp.float32)
    centred = widened - jnp.mean(widened, -1, keepdims=True)
    return (
        centred * lax.rsqrt(jnp.mean(centred * centred, -1, keepdims=True) + layer_eps) * gain
    ).astype(jnp.bfloat16)


def rotary_tables(positions):
    halfway = ROPE_DIM // 2
    inverse = rotary_base ** (-(jnp.arange(halfway, dtype=jnp.float32) * 2.0 / ROPE_DIM))
    angles = positions.astype(jnp.float32)[:, None] * inverse[None, :]
    return (jnp.cos(angles), jnp.sin(angles))


def rotate(values, cosine_table, sine_table):
    halfway = values.shape[-1] // 2
    first_half = values[..., :halfway]
    second_half = values[..., halfway:]
    return jnp.concatenate(
        [
            first_half * cosine_table - second_half * sine_table,
            second_half * cosine_table + first_half * sine_table,
        ],
        -1,
    )


def block_stats(query_block, query_pos, keyvals, rotated_keys, key_pos):
    scale = float(NOPE + ROPE_DIM) ** (-0.5)
    scores = jnp.einsum(
        "qhd,khd->hqk",
        query_block[..., :NOPE],
        keyvals[..., :NOPE],
        preferred_element_type=jnp.float32,
    )
    scores = (
        scores
        + jnp.einsum(
            "qhd,kd->hqk", query_block[..., NOPE:], rotated_keys, preferred_element_type=jnp.float32
        )
    ) * scale
    allowed = key_pos[None, :] <= query_pos[:, None]
    scores = jnp.where(allowed[None], scores, -jnp.inf)
    block_max = jnp.max(scores, -1)
    weights = jnp.exp(scores - block_max[..., None])
    block_sum = jnp.sum(weights, -1)
    attended = jnp.einsum(
        "hqk,khd->qhd",
        weights.astype(jnp.bfloat16),
        keyvals[..., NOPE:],
        preferred_element_type=jnp.float32,
    ).astype(jnp.bfloat16)
    return (block_max.T, block_sum.T, attended)


def merge_block(carried, stats):
    running_max, running_sum, running_acc = carried
    block_max, block_sum, attended = stats
    new_max = jnp.maximum(running_max, block_max)
    old_weight = jnp.exp(running_max - new_max)
    new_weight = jnp.exp(block_max - new_max)
    return (
        new_max,
        running_sum * old_weight + block_sum * new_weight,
        running_acc * old_weight[..., None] + attended.astype(jnp.float32) * new_weight[..., None],
    )


def body(
    q_latent,
    kv_latent,
    rope_key,
    q_gain,
    kv_gain,
    w_query,
    w_keyval,
    w_output,
    moe_input,
    moe_gain,
    routes,
    route_weight,
    expert_gate,
    expert_up,
    expert_down,
    shared_gate,
    shared_up,
    shared_down,
):
    row_count = q_latent.shape[0]
    own_index = lax.axis_index("ep")
    ep_count = lax.axis_size("ep")
    tp_count = lax.axis_size("tp")
    positions = own_index * row_count + jnp.arange(row_count, dtype=jnp.int32)
    cosine_table, sine_table = rotary_tables(positions)
    q_normed = rms_scale(q_latent, q_gain)
    kv_normed = rms_scale(kv_latent, kv_gain)
    key_rotated = rotate(rope_key.astype(jnp.float32), cosine_table, sine_table).astype(
        jnp.bfloat16
    )
    heads_local = w_query.shape[1] // (NOPE + ROPE_DIM)
    projected = jnp.dot(q_normed, w_query, preferred_element_type=jnp.float32)
    projected = projected.reshape(row_count, heads_local, NOPE + ROPE_DIM)
    queries = jnp.concatenate(
        [
            projected[..., :NOPE],
            rotate(projected[..., NOPE:], cosine_table[:, None, :], sine_table[:, None, :]),
        ],
        -1,
    ).astype(jnp.bfloat16)

    def expand_keys(latent_rows):
        expanded = jnp.dot(latent_rows, w_keyval, preferred_element_type=jnp.float32).astype(
            jnp.bfloat16
        )
        return expanded.reshape(latent_rows.shape[0], heads_local, NOPE + VDIM)

    initial = (
        jnp.full((row_count, heads_local), floor_value, jnp.float32),
        jnp.zeros((row_count, heads_local), jnp.float32),
        jnp.zeros((row_count, heads_local, VDIM), jnp.float32),
    )
    carried = initial
    latent_piece = lax.all_gather(kv_normed, "ep", axis=0, tiled=True)
    rotated_piece = lax.all_gather(key_rotated, "ep", axis=0, tiled=True)
    block_count = latent_piece.shape[0] // row_count

    def visit_block(inner, offset):

        def live(current):
            latent_rows = lax.dynamic_slice_in_dim(latent_piece, offset * row_count, row_count, 0)
            rotated_rows = lax.dynamic_slice_in_dim(rotated_piece, offset * row_count, row_count, 0)
            key_pos = offset * row_count + jnp.arange(row_count, dtype=jnp.int32)
            stats = block_stats(queries, positions, expand_keys(latent_rows), rotated_rows, key_pos)
            return merge_block(current, stats)

        def skipped(current):
            return current

        return (lax.cond(offset <= own_index, live, skipped, inner), None)

    carried, unused = lax.scan(visit_block, carried, jnp.arange(block_count, dtype=jnp.int32))
    running_max, running_sum, running_acc = carried
    heads_out = (
        (running_acc / running_sum[..., None])
        .astype(jnp.bfloat16)
        .reshape(row_count, heads_local * VDIM)
    )
    mixed = jnp.dot(
        lax.all_gather(heads_out, "tp", axis=1, tiled=True),
        w_output,
        preferred_element_type=jnp.float32,
    )
    mixed = mixed.astype(jnp.bfloat16)
    width = moe_input.shape[1]
    top_count = routes.shape[1]
    local_experts = expert_gate.shape[0]
    expert_count = local_experts * ep_count
    capacity = max(2, 3 * MOE_DEV * top_count // (2 * expert_count))
    normed = layer_scale(moe_input, moe_gain)
    entries = routes.reshape(tp_count, MOE_DEV * top_count)
    onehot = (entries[..., None] == jnp.arange(expert_count, dtype=jnp.int32)).astype(jnp.int32)
    earlier = jnp.cumsum(onehot, 1) - onehot
    rank_in = jnp.sum(earlier * onehot, -1)
    block_ids = jnp.arange(tp_count, dtype=jnp.int32)[:, None]
    slot_of = ((entries * tp_count + block_ids) * capacity + rank_in).reshape(-1, top_count)
    token_ids = jnp.arange(tp_count * MOE_DEV * top_count, dtype=jnp.int32) // top_count
    slot_token = (
        jnp.full((expert_count * tp_count * capacity,), -1, jnp.int32)
        .at[slot_of.reshape(-1)]
        .set(token_ids)
    )
    outgoing = jnp.where(
        (slot_token >= 0)[:, None], normed[jnp.maximum(slot_token, 0)], jnp.zeros((), jnp.bfloat16)
    )
    outgoing = outgoing.reshape(ep_count, local_experts, tp_count, capacity, width)
    arrived = lax.all_to_all(outgoing, "ep", split_axis=0, concat_axis=0, tiled=True)
    slot_rows = arrived.shape[3]
    inputs = arrived[:, 0].reshape(-1, width)
    hidden = jax.nn.silu(jnp.dot(inputs, expert_gate[0], preferred_element_type=jnp.float32))
    hidden = (hidden * jnp.dot(inputs, expert_up[0], preferred_element_type=jnp.float32)).astype(
        jnp.bfloat16
    )
    output = jnp.dot(hidden, expert_down[0], preferred_element_type=jnp.float32)
    results = [output.astype(jnp.bfloat16).reshape(ep_count, tp_count, slot_rows, width)]
    partial_value = jnp.stack(results, 1)
    shared_hidden = jax.nn.silu(jnp.dot(normed, shared_gate, preferred_element_type=jnp.float32))
    shared_hidden = (
        shared_hidden * jnp.dot(normed, shared_up, preferred_element_type=jnp.float32)
    ).astype(jnp.bfloat16)
    shared_part = jnp.dot(shared_hidden, shared_down, preferred_element_type=jnp.float32).astype(
        jnp.bfloat16
    )
    slot_total, shared_total = (
        lax.psum_scatter(
            partial_value.astype(jnp.float32).astype(jnp.bfloat16),
            "tp",
            scatter_dimension=2,
            tiled=True,
        ).astype(jnp.float32),
        lax.psum_scatter(
            shared_part.astype(jnp.float32)
            .reshape(1, 1, tp_count, MOE_DEV, width)
            .astype(jnp.bfloat16),
            "tp",
            scatter_dimension=2,
            tiled=True,
        ).astype(jnp.float32),
    )
    arrived_sums = lax.all_to_all(
        slot_total.astype(jnp.bfloat16), "ep", split_axis=0, concat_axis=0, tiled=True
    ).astype(slot_total.dtype)
    own_block = lax.axis_index("tp")
    own_entries = lax.dynamic_slice_in_dim(routes, own_block * MOE_DEV, MOE_DEV, 0)
    own_rank = lax.dynamic_slice_in_dim(
        rank_in.reshape(-1, top_count), own_block * MOE_DEV, MOE_DEV, 0
    )
    own_weight = lax.dynamic_slice_in_dim(route_weight, own_block * MOE_DEV, MOE_DEV, 0)
    picked = arrived_sums.reshape(-1, width)[own_entries * capacity + own_rank]
    moe_out = (
        jnp.sum(own_weight[..., None] * picked, 1) + shared_total.reshape(MOE_DEV, width)
    ).astype(jnp.bfloat16)
    return (mixed, moe_out)


def move(value, ep_flip, tp_flip):
    ep_count = lax.axis_size("ep")
    tp_count = lax.axis_size("tp")
    pairs = [
        (e * tp_count + t, (e ^ ep_flip) * tp_count + (t ^ tp_flip))
        for e in range(ep_count)
        for t in range(tp_count)
    ]
    return lax.ppermute(value, ("ep", "tp"), pairs)


LANES = 128
LOG2E = 1.4426950408889634


def attention_kernel(heads, others, scale, ep_ref, *refs):
    q_ref, wq_ref, cos_ref, sin_ref, local_ref = refs[:5]
    mine = refs[5 : 5 + others]
    theirs = refs[5 + others : 5 + 2 * others]
    wkv_ref, out_ref, k_ref, v_ref = refs[5 + 2 * others :]
    own = ep_ref[0]
    index = pl.program_id(0)
    rows = q_ref.shape[0]
    row_count, packed = local_ref.shape
    latent = packed - LANES
    half = row_count // 2
    factor = scale * LOG2E

    def expand(piece, start):
        values = piece[...]
        lane = lax.broadcasted_iota(jnp.int32, (values.shape[0], LANES), 1)
        product = jnp.dot(
            values[:, :latent], wkv_ref[...], preferred_element_type=jnp.float32
        ).astype(jnp.bfloat16)
        for head in range(heads):
            pair = product[:, head * LANES : (head + 1) * LANES]
            k_ref[head, start : start + values.shape[0], :] = jnp.where(
                lane < NOPE, pair, values[:, latent:]
            )
            v_ref[head, start : start + values.shape[0], :] = jnp.where(
                lane == 0, jnp.ones_like(pair), pair
            )

    @pl.when(index == 0)
    def _():
        expand(local_ref, 0)
        for k in range(1, others + 1):

            @pl.when(lax.bitwise_xor(own, jnp.int32(k)) < own)
            def _(k=k):
                expand(mine[k - 1], k * row_count)
                expand(theirs[k - 1], k * row_count + half)

    projected = jnp.dot(q_ref[...], wq_ref[...], preferred_element_type=jnp.float32)
    queries = []
    for head in range(heads):
        straight = projected[:, head * LANES : (head + 1) * LANES]
        swapped = projected[:, (heads + head) * LANES : (heads + head + 1) * LANES]
        queries.append((straight * cos_ref[...] + swapped * sin_ref[...]).astype(jnp.bfloat16))

    def attend(carry, start, width, masked):
        scored = [
            lax.dot_general(
                queries[head],
                k_ref[head, pl.ds(start, width), :],
                (((1,), (1,)), ((), ())),
                preferred_element_type=jnp.float32,
            )
            for head in range(heads)
        ]
        result = []
        for head in range(heads):
            scores = scored[head]
            old_max, acc = carry[head]
            if masked:
                row = lax.broadcasted_iota(jnp.int32, scores.shape, 0)
                column = lax.broadcasted_iota(jnp.int32, scores.shape, 1)
                scores = jnp.where(column <= row, scores, -jnp.inf)
            new_max = jnp.maximum(old_max, jnp.max(scores, -1, keepdims=True))
            weights = jnp.exp2((scores - new_max) * factor).astype(jnp.bfloat16)
            product = jnp.dot(
                weights, v_ref[head, pl.ds(start, width), :], preferred_element_type=jnp.float32
            )
            result.append((new_max, acc * jnp.exp2((old_max - new_max) * factor) + product))
        return tuple(result)

    carry = tuple(
        (jnp.full((rows, 1), floor_value, jnp.float32), jnp.zeros((rows, LANES), jnp.float32))
        for head in range(heads)
    )
    carry = attend(carry, pl.multiple_of(index * rows, rows), rows, True)
    carry = lax.fori_loop(
        0, index, lambda i, c: attend(c, pl.multiple_of(i * rows, rows), rows, False), carry
    )

    def remote(source, c):
        start = lax.bitwise_xor(own, source) * row_count
        return attend(c, pl.multiple_of(start, row_count), row_count, False)

    carry = lax.fori_loop(0, own, remote, carry)
    outs = [acc[:, NOPE : NOPE + VDIM] / acc[:, :1] for _, acc in carry]
    out_ref[...] = jnp.concatenate(outs, -1).astype(jnp.bfloat16)


def flash(own_index, q_normed, wq, cosine, sine, local, mine, theirs, w_keyval):
    heads = w_keyval.shape[1] // (NOPE + VDIM)
    others = len(mine)
    row_count, packed = local.shape
    tile = min(256, row_count)
    total = row_count * (others + 1)
    scale = float(NOPE + ROPE_DIM) ** (-0.5)

    def whole(array):
        return pl.BlockSpec(array.shape, lambda i, s: (0, 0))

    def tiled(array):
        return pl.BlockSpec((tile, array.shape[1]), lambda i, s: (i, 0))

    operands = (q_normed, wq, cosine, sine, local, *mine, *theirs, w_keyval)
    return pl.pallas_call(
        lambda *refs: attention_kernel(heads, others, scale, *refs),
        out_shape=jax.ShapeDtypeStruct((row_count, heads * VDIM), jnp.bfloat16),
        grid_spec=pltpu.PrefetchScalarGridSpec(
            num_scalar_prefetch=1,
            grid=(row_count // tile,),
            in_specs=[tiled(q_normed), whole(wq), tiled(cosine), tiled(sine)]
            + [whole(x) for x in operands[4:]],
            out_specs=pl.BlockSpec((tile, heads * VDIM), lambda i, s: (i, 0)),
            scratch_shapes=[
                pltpu.VMEM((heads, total, LANES), jnp.bfloat16),
                pltpu.VMEM((heads, total, LANES), jnp.bfloat16),
            ],
        ),
        cost_estimate=pl.CostEstimate(
            flops=4 * heads * row_count * total * LANES,
            bytes_accessed=4 * total * packed,
            transcendentals=heads * row_count * total,
        ),
        compiler_params=pltpu.CompilerParams(vmem_limit_bytes=40 * 1024 * 1024),
        name="attend",
    )(own_index.astype(jnp.int32).reshape(1), *operands)


def expert_kernel(count, steps, with_addend, *refs):
    pieces = refs[:count]
    gate_ref, up_ref, down_ref = refs[count : count + 3]
    rest = refs[count + 3 :]
    if with_addend:
        addend_ref, rest = rest[0], rest[1:]
    outs, (x_ref, total_ref) = rest[:-2], rest[-2:]
    step = pl.program_id(0)
    block = pieces[0].shape[0]

    @pl.when(step == 0)
    def _():
        for i in range(count):
            x_ref[i * block : (i + 1) * block, :] = pieces[i][...]

    inputs = x_ref[...]
    hidden = jnp.dot(inputs, gate_ref[...], preferred_element_type=jnp.float32)
    hidden = hidden / (1.0 + jnp.exp(-hidden))
    hidden = hidden * jnp.dot(inputs, up_ref[...], preferred_element_type=jnp.float32)
    product = jnp.dot(
        hidden.astype(jnp.bfloat16), down_ref[...], preferred_element_type=jnp.float32
    )

    @pl.when(step == 0)
    def _():
        total_ref[...] = product

    @pl.when(step > 0)
    def _():
        total_ref[...] += product

    @pl.when(step == steps - 1)
    def _():
        size = outs[0].shape[0]
        for i, out in enumerate(outs):
            value = total_ref[i * size : (i + 1) * size, :]
            if with_addend:
                value = value.astype(jnp.bfloat16).astype(jnp.float32)
                value = value + addend_ref[i * size : (i + 1) * size, :].astype(jnp.float32)
            out[...] = value.astype(jnp.bfloat16)


def expert_call(pieces, gate, up, down, addend):
    count = len(pieces)
    block, width = pieces[0].shape
    rows = count * block
    hidden = gate.shape[1]
    tile = min(256, hidden)
    steps = hidden // tile
    split = addend is not None
    outs = count if split else 1
    full = lambda shape: pl.BlockSpec(shape, lambda i: (0, 0))
    operands = (*pieces, gate, up, down) + ((addend,) if split else ())
    result = pl.pallas_call(
        lambda *refs: expert_kernel(count, steps, split, *refs),
        out_shape=[jax.ShapeDtypeStruct((rows // outs, width), jnp.bfloat16)] * outs,
        grid=(steps,),
        in_specs=[full((block, width))] * count
        + [
            pl.BlockSpec((width, tile), lambda i: (0, i)),
            pl.BlockSpec((width, tile), lambda i: (0, i)),
            pl.BlockSpec((tile, width), lambda i: (i, 0)),
        ]
        + ([full((rows, width))] if split else []),
        out_specs=[full((rows // outs, width))] * outs,
        scratch_shapes=[
            pltpu.VMEM((rows, width), jnp.bfloat16),
            pltpu.VMEM((rows, width), jnp.float32),
        ],
        cost_estimate=pl.CostEstimate(
            flops=6 * rows * width * hidden,
            bytes_accessed=6 * width * hidden + 4 * rows * width,
            transcendentals=rows * hidden,
        ),
        compiler_params=pltpu.CompilerParams(vmem_limit_bytes=40 * 1024 * 1024),
        name="experts_sum" if split else "experts",
    )(*operands)
    return result if split else result[0]


def dense_body(
    q_latent,
    kv_latent,
    rope_key,
    q_gain,
    kv_gain,
    w_query,
    w_keyval,
    w_output,
    moe_input,
    moe_gain,
    routes,
    route_weight,
    expert_gate,
    expert_up,
    expert_down,
    shared_gate,
    shared_up,
    shared_down,
):
    row_count = q_latent.shape[0]
    half = row_count // 2
    own = lax.axis_index("ep")
    ep_count = lax.axis_size("ep")
    tp_count = lax.axis_size("tp")
    tp_index = lax.axis_index("tp")
    core = tp_index % 2
    depth = tp_index // 2
    depth_count = tp_count // 2
    width = moe_input.shape[1]
    heads_local = w_query.shape[1] // (NOPE + ROPE_DIM)
    halfway = ROPE_DIM // 2
    positions = own * row_count + jnp.arange(row_count, dtype=jnp.int32)
    inverse = rotary_base ** (-(jnp.arange(halfway, dtype=jnp.float32) * 2.0 / ROPE_DIM))
    spread = jnp.concatenate(
        [
            jnp.zeros((NOPE,), jnp.float32),
            inverse,
            inverse,
            jnp.zeros((LANES - NOPE - ROPE_DIM,), jnp.float32),
        ]
    )
    angles = positions.astype(jnp.float32)[:, None] * spread[None, :]
    lane = jnp.arange(LANES)
    cosine = jnp.cos(angles)
    sine = jnp.sin(angles) * jnp.where(lane < NOPE + halfway, -1.0, 1.0)[None, :]

    def exchange(index):
        rope = (index >= NOPE) & (index < NOPE + ROPE_DIM)
        return np.where(rope, NOPE + (index - NOPE + halfway) % ROPE_DIM, -1)

    lanes = np.arange(LANES)
    straight = np.where(lanes < NOPE + ROPE_DIM, lanes, -1)
    swapped = exchange(lanes)
    one_head = np.arange(NOPE + ROPE_DIM)
    pick_straight = np.kron(np.eye(heads_local), one_head[:, None] == straight[None, :])
    pick_swapped = np.kron(np.eye(heads_local), one_head[:, None] == swapped[None, :])
    pick_query = jnp.asarray(np.concatenate([pick_straight, pick_swapped], 1), jnp.bfloat16)
    rope_lane = np.arange(NOPE, NOPE + ROPE_DIM)
    pick_key = jnp.asarray(rope_lane[:, None] == straight[None, :], jnp.bfloat16)
    pick_key_swapped = jnp.asarray(rope_lane[:, None] == swapped[None, :], jnp.bfloat16)

    kv_normed = rms_scale(kv_latent, kv_gain)
    key_rotated = (
        jnp.dot(rope_key, pick_key, preferred_element_type=jnp.float32) * cosine
        + jnp.dot(rope_key, pick_key_swapped, preferred_element_type=jnp.float32) * sine
    ).astype(jnp.bfloat16)
    local_pack = jnp.concatenate([kv_normed, key_rotated], 1)
    sent_pack = lax.dynamic_slice_in_dim(local_pack, core * half, half, 0)
    packs_mine = [move(sent_pack, k, 0) for k in range(1, ep_count)]
    packs_other = [move(pack, 0, 1) for pack in packs_mine]

    grouped = moe_input.reshape(depth_count, 2, MOE_DEV, width)
    own_rows = layer_scale(
        lax.dynamic_index_in_dim(grouped, core, 1, keepdims=False).reshape(-1, width), moe_gain
    )
    other_rows = layer_scale(
        lax.dynamic_index_in_dim(grouped, 1 - core, 1, keepdims=False).reshape(-1, width), moe_gain
    )
    block_rows = own_rows.shape[0]
    arrived = [move(own_rows, k, 0) for k in range(1, ep_count)]
    swapped_rows = [move(piece, 0, 1) for piece in arrived]

    q_normed = rms_scale(q_latent, q_gain)
    spread_query = jnp.dot(w_query, pick_query, preferred_element_type=jnp.float32).astype(
        jnp.bfloat16
    )
    heads_out = flash(
        own, q_normed, spread_query, cosine, sine, local_pack, packs_mine, packs_other, w_keyval
    )

    head_parts = [heads_out] + [move(heads_out, 0, 2 * k) for k in range(1, depth_count)]
    heads_mine = jnp.concatenate(head_parts, 1)
    heads_other = move(heads_mine, 0, 1)
    head_rows = heads_local * VDIM

    def output_rows(side):
        return jnp.concatenate(
            [
                lax.dynamic_slice_in_dim(
                    w_output, (2 * jnp.bitwise_xor(depth, k) + side) * head_rows, head_rows, 0
                )
                for k in range(depth_count)
            ],
            0,
        )

    mixed = (
        jnp.dot(heads_mine, output_rows(core), preferred_element_type=jnp.float32)
        + jnp.dot(heads_other, output_rows(1 - core), preferred_element_type=jnp.float32)
    ).astype(jnp.bfloat16)

    def gated(inputs, gate, up, down):
        hidden = jax.nn.silu(jnp.dot(inputs, gate, preferred_element_type=jnp.float32))
        hidden = (hidden * jnp.dot(inputs, up, preferred_element_type=jnp.float32)).astype(
            jnp.bfloat16
        )
        return jnp.dot(hidden, down, preferred_element_type=jnp.float32).astype(jnp.bfloat16)

    shared_both = gated(
        jnp.concatenate([own_rows, other_rows], 0), shared_gate, shared_up, shared_down
    )
    shared_swapped = move(shared_both[block_rows:], 0, 1)
    routed_inputs, _ = lax.optimization_barrier(
        ((own_rows, other_rows, arrived, swapped_rows), heads_out)
    )
    own_rows, other_rows, arrived, swapped_rows = routed_inputs
    weights = (expert_gate[0], expert_up[0], expert_down[0])
    routed_other = expert_call([other_rows] + swapped_rows, *weights, None)
    routed_swapped = move(routed_other, 0, 1)
    pair_sum = expert_call([own_rows] + arrived, *weights, routed_swapped)
    returned = [pair_sum[0]] + [move(pair_sum[k], k, 0) for k in range(1, ep_count)]
    own_routes = lax.dynamic_index_in_dim(
        routes.reshape(depth_count, 2, MOE_DEV, -1), core, 1, keepdims=False
    ).reshape(block_rows, -1)
    own_weight = lax.dynamic_index_in_dim(
        route_weight.reshape(depth_count, 2, MOE_DEV, -1), core, 1, keepdims=False
    ).reshape(block_rows, -1)
    summed = shared_both[:block_rows].astype(jnp.float32) + shared_swapped.astype(jnp.float32)
    for k in range(ep_count):
        weight = jnp.sum(
            jnp.where(own_routes == jnp.bitwise_xor(own, k), own_weight, 0.0), -1, keepdims=True
        )
        summed = summed + weight * returned[k].astype(jnp.float32)
    summed = summed.astype(jnp.bfloat16).reshape(depth_count, MOE_DEV, width)
    moe_out = lax.dynamic_index_in_dim(summed, depth, 0, keepdims=False).astype(jnp.float32)
    for k in range(1, depth_count):
        part = lax.dynamic_index_in_dim(summed, jnp.bitwise_xor(depth, k), 0, keepdims=False)
        moe_out = moe_out + move(part, 0, 2 * k).astype(jnp.float32)
    return (mixed, moe_out.astype(jnp.bfloat16))


def solution(mesh):
    in_specs = (
        P("ep", None),
        P("ep", None),
        P("ep", None),
        P(),
        P(),
        P(None, "tp"),
        P(None, "tp"),
        P(None, "tp"),
        P("ep", None),
        P(),
        P("ep", None),
        P("ep", None),
        P("ep", None, "tp"),
        P("ep", None, "tp"),
        P("ep", "tp", None),
        P(None, "tp"),
        P(None, "tp"),
        P("tp", None),
    )
    out_specs = (P("ep", "tp"), P(("ep", "tp"), None))
    dense = mesh.shape["ep"] <= 4
    return jax.shard_map(dense_body if dense else body, mesh=mesh, in_specs=in_specs, out_specs=out_specs, check_vma=False)
```

```python
import jax
import jax.numpy as jnp
import numpy as np
from jax import lax
from jax.experimental import pallas as pl
from jax.experimental.pallas import tpu as pltpu
from jax.sharding import PartitionSpec as P


NOPE = 64
ROPE_DIM = 32
VDIM = 64
MOE_DEV = 32


norm_eps = 1e-06
layer_eps = 1e-05
rotary_base = 10000.0
floor_value = -1e30


def rms_scale(values, gain):
    widened = values.astype(jnp.float32)
    return (
        widened * lax.rsqrt(jnp.mean(widened * widened, -1, keepdims=True) + norm_eps) * gain
    ).astype(jnp.bfloat16)


def layer_scale(values, gain):
    widened = values.astype(jnp.float32)
    centred = widened - jnp.mean(widened, -1, keepdims=True)
    return (
        centred * lax.rsqrt(jnp.mean(centred * centred, -1, keepdims=True) + layer_eps) * gain
    ).astype(jnp.bfloat16)


def rotary_tables(positions):
    halfway = ROPE_DIM // 2
    inverse = rotary_base ** (-(jnp.arange(halfway, dtype=jnp.float32) * 2.0 / ROPE_DIM))
    angles = positions.astype(jnp.float32)[:, None] * inverse[None, :]
    return (jnp.cos(angles), jnp.sin(angles))


def rotate(values, cosine_table, sine_table):
    halfway = values.shape[-1] // 2
    first_half = values[..., :halfway]
    second_half = values[..., halfway:]
    return jnp.concatenate(
        [
            first_half * cosine_table - second_half * sine_table,
            second_half * cosine_table + first_half * sine_table,
        ],
        -1,
    )


def block_stats(query_block, query_pos, keyvals, rotated_keys, key_pos):
    scale = float(NOPE + ROPE_DIM) ** (-0.5)
    scores = jnp.einsum(
        "qhd,khd->hqk",
        query_block[..., :NOPE],
        keyvals[..., :NOPE],
        preferred_element_type=jnp.float32,
    )
    scores = (
        scores
        + jnp.einsum(
            "qhd,kd->hqk", query_block[..., NOPE:], rotated_keys, preferred_element_type=jnp.float32
        )
    ) * scale
    allowed = key_pos[None, :] <= query_pos[:, None]
    scores = jnp.where(allowed[None], scores, -jnp.inf)
    block_max = jnp.max(scores, -1)
    weights = jnp.exp(scores - block_max[..., None])
    block_sum = jnp.sum(weights, -1)
    attended = jnp.einsum(
        "hqk,khd->qhd",
        weights.astype(jnp.bfloat16),
        keyvals[..., NOPE:],
        preferred_element_type=jnp.float32,
    ).astype(jnp.bfloat16)
    return (block_max.T, block_sum.T, attended)


def merge_block(carried, stats):
    running_max, running_sum, running_acc = carried
    block_max, block_sum, attended = stats
    new_max = jnp.maximum(running_max, block_max)
    old_weight = jnp.exp(running_max - new_max)
    new_weight = jnp.exp(block_max - new_max)
    return (
        new_max,
        running_sum * old_weight + block_sum * new_weight,
        running_acc * old_weight[..., None] + attended.astype(jnp.float32) * new_weight[..., None],
    )


def body(
    q_latent,
    kv_latent,
    rope_key,
    q_gain,
    kv_gain,
    w_query,
    w_keyval,
    w_output,
    moe_input,
    moe_gain,
    routes,
    route_weight,
    expert_gate,
    expert_up,
    expert_down,
    shared_gate,
    shared_up,
    shared_down,
):
    row_count = q_latent.shape[0]
    own_index = lax.axis_index("ep")
    ep_count = lax.axis_size("ep")
    tp_count = lax.axis_size("tp")
    positions = own_index * row_count + jnp.arange(row_count, dtype=jnp.int32)
    cosine_table, sine_table = rotary_tables(positions)
    q_normed = rms_scale(q_latent, q_gain)
    kv_normed = rms_scale(kv_latent, kv_gain)
    key_rotated = rotate(rope_key.astype(jnp.float32), cosine_table, sine_table).astype(
        jnp.bfloat16
    )
    heads_local = w_query.shape[1] // (NOPE + ROPE_DIM)
    projected = jnp.dot(q_normed, w_query, preferred_element_type=jnp.float32)
    projected = projected.reshape(row_count, heads_local, NOPE + ROPE_DIM)
    queries = jnp.concatenate(
        [
            projected[..., :NOPE],
            rotate(projected[..., NOPE:], cosine_table[:, None, :], sine_table[:, None, :]),
        ],
        -1,
    ).astype(jnp.bfloat16)

    def expand_keys(latent_rows):
        expanded = jnp.dot(latent_rows, w_keyval, preferred_element_type=jnp.float32).astype(
            jnp.bfloat16
        )
        return expanded.reshape(latent_rows.shape[0], heads_local, NOPE + VDIM)

    initial = (
        jnp.full((row_count, heads_local), floor_value, jnp.float32),
        jnp.zeros((row_count, heads_local), jnp.float32),
        jnp.zeros((row_count, heads_local, VDIM), jnp.float32),
    )
    carried = initial
    latent_piece = lax.all_gather(kv_normed, "ep", axis=0, tiled=True)
    rotated_piece = lax.all_gather(key_rotated, "ep", axis=0, tiled=True)
    block_count = latent_piece.shape[0] // row_count

    def visit_block(inner, offset):

        def live(current):
            latent_rows = lax.dynamic_slice_in_dim(latent_piece, offset * row_count, row_count, 0)
            rotated_rows = lax.dynamic_slice_in_dim(rotated_piece, offset * row_count, row_count, 0)
            key_pos = offset * row_count + jnp.arange(row_count, dtype=jnp.int32)
            stats = block_stats(queries, positions, expand_keys(latent_rows), rotated_rows, key_pos)
            return merge_block(current, stats)

        def skipped(current):
            return current

        return (lax.cond(offset <= own_index, live, skipped, inner), None)

    carried, _ = lax.scan(visit_block, carried, jnp.arange(block_count, dtype=jnp.int32))
    _, running_sum, running_acc = carried
    heads_out = (
        (running_acc / running_sum[..., None])
        .astype(jnp.bfloat16)
        .reshape(row_count, heads_local * VDIM)
    )
    mixed = jnp.dot(
        lax.all_gather(heads_out, "tp", axis=1, tiled=True),
        w_output,
        preferred_element_type=jnp.float32,
    )
    mixed = mixed.astype(jnp.bfloat16)
    width = moe_input.shape[1]
    top_count = routes.shape[1]
    local_experts = expert_gate.shape[0]
    expert_count = local_experts * ep_count
    capacity = max(2, 3 * MOE_DEV * top_count // (2 * expert_count))
    normed = layer_scale(moe_input, moe_gain)
    entries = routes.reshape(tp_count, MOE_DEV * top_count)
    onehot = (entries[..., None] == jnp.arange(expert_count, dtype=jnp.int32)).astype(jnp.int32)
    earlier = jnp.cumsum(onehot, 1) - onehot
    rank_in = jnp.sum(earlier * onehot, -1)
    block_ids = jnp.arange(tp_count, dtype=jnp.int32)[:, None]
    slot_of = ((entries * tp_count + block_ids) * capacity + rank_in).reshape(-1, top_count)
    token_ids = jnp.arange(tp_count * MOE_DEV * top_count, dtype=jnp.int32) // top_count
    slot_token = (
        jnp.full((expert_count * tp_count * capacity,), -1, jnp.int32)
        .at[slot_of.reshape(-1)]
        .set(token_ids)
    )
    outgoing = jnp.where(
        (slot_token >= 0)[:, None], normed[jnp.maximum(slot_token, 0)], jnp.zeros((), jnp.bfloat16)
    )
    outgoing = outgoing.reshape(ep_count, local_experts, tp_count, capacity, width)
    arrived = lax.all_to_all(outgoing, "ep", split_axis=0, concat_axis=0, tiled=True)
    slot_rows = arrived.shape[3]
    inputs = arrived[:, 0].reshape(-1, width)
    hidden = jax.nn.silu(jnp.dot(inputs, expert_gate[0], preferred_element_type=jnp.float32))
    hidden = (hidden * jnp.dot(inputs, expert_up[0], preferred_element_type=jnp.float32)).astype(
        jnp.bfloat16
    )
    output = jnp.dot(hidden, expert_down[0], preferred_element_type=jnp.float32)
    results = [output.astype(jnp.bfloat16).reshape(ep_count, tp_count, slot_rows, width)]
    partial_value = jnp.stack(results, 1)
    shared_hidden = jax.nn.silu(jnp.dot(normed, shared_gate, preferred_element_type=jnp.float32))
    shared_hidden = (
        shared_hidden * jnp.dot(normed, shared_up, preferred_element_type=jnp.float32)
    ).astype(jnp.bfloat16)
    shared_part = jnp.dot(shared_hidden, shared_down, preferred_element_type=jnp.float32).astype(
        jnp.bfloat16
    )
    slot_total, shared_total = (
        lax.psum_scatter(
            partial_value.astype(jnp.float32).astype(jnp.bfloat16),
            "tp",
            scatter_dimension=2,
            tiled=True,
        ).astype(jnp.float32),
        lax.psum_scatter(
            shared_part.astype(jnp.float32)
            .reshape(1, 1, tp_count, MOE_DEV, width)
            .astype(jnp.bfloat16),
            "tp",
            scatter_dimension=2,
            tiled=True,
        ).astype(jnp.float32),
    )
    arrived_sums = lax.all_to_all(
        slot_total.astype(jnp.bfloat16), "ep", split_axis=0, concat_axis=0, tiled=True
    ).astype(slot_total.dtype)
    own_block = lax.axis_index("tp")
    own_entries = lax.dynamic_slice_in_dim(routes, own_block * MOE_DEV, MOE_DEV, 0)
    own_rank = lax.dynamic_slice_in_dim(
        rank_in.reshape(-1, top_count), own_block * MOE_DEV, MOE_DEV, 0
    )
    own_weight = lax.dynamic_slice_in_dim(route_weight, own_block * MOE_DEV, MOE_DEV, 0)
    picked = arrived_sums.reshape(-1, width)[own_entries * capacity + own_rank]
    moe_out = (
        jnp.sum(own_weight[..., None] * picked, 1) + shared_total.reshape(MOE_DEV, width)
    ).astype(jnp.bfloat16)
    return (mixed, moe_out)


def move(value, ep_flip, tp_flip):
    ep_count = lax.axis_size("ep")
    tp_count = lax.axis_size("tp")
    pairs = [
        (e * tp_count + t, (e ^ ep_flip) * tp_count + (t ^ tp_flip))
        for e in range(ep_count)
        for t in range(tp_count)
    ]
    return lax.ppermute(value, ("ep", "tp"), pairs)


LANES = 128
LOG2E = 1.4426950408889634


def attention_kernel(heads, others, scale, ep_ref, *refs):
    q_ref, wq_ref, cos_ref, sin_ref, local_ref = refs[:5]
    mine = refs[5 : 5 + others]
    theirs = refs[5 + others : 5 + 2 * others]
    wkv_ref, out_ref, k_ref, v_ref = refs[5 + 2 * others :]
    own = ep_ref[0]
    index = pl.program_id(0)
    rows = q_ref.shape[0]
    row_count, packed = local_ref.shape
    latent = packed - LANES
    half = row_count // 2
    factor = scale * LOG2E

    def expand(piece, start):
        values = piece[...]
        lane = lax.broadcasted_iota(jnp.int32, (values.shape[0], LANES), 1)
        product = jnp.dot(
            values[:, :latent], wkv_ref[...], preferred_element_type=jnp.float32
        ).astype(jnp.bfloat16)
        for head in range(heads):
            pair = product[:, head * LANES : (head + 1) * LANES]
            k_ref[head, start : start + values.shape[0], :] = jnp.where(
                lane < NOPE, pair, values[:, latent:]
            )
            v_ref[head, start : start + values.shape[0], :] = jnp.where(
                lane == 0, jnp.ones_like(pair), pair
            )

    @pl.when(index == 0)
    def _():
        expand(local_ref, 0)
        for k in range(1, others + 1):

            @pl.when(lax.bitwise_xor(own, jnp.int32(k)) < own)
            def _(k=k):
                expand(mine[k - 1], k * row_count)
                expand(theirs[k - 1], k * row_count + half)

    projected = jnp.dot(q_ref[...], wq_ref[...], preferred_element_type=jnp.float32)
    queries = []
    for head in range(heads):
        straight = projected[:, head * LANES : (head + 1) * LANES]
        swapped = projected[:, (heads + head) * LANES : (heads + head + 1) * LANES]
        queries.append((straight * cos_ref[...] + swapped * sin_ref[...]).astype(jnp.bfloat16))

    def attend(carry, start, width, masked):
        scored = [
            lax.dot_general(
                queries[head],
                k_ref[head, pl.ds(start, width), :],
                (((1,), (1,)), ((), ())),
                preferred_element_type=jnp.float32,
            )
            for head in range(heads)
        ]
        result = []
        for head in range(heads):
            scores = scored[head]
            old_max, acc = carry[head]
            if masked:
                row = lax.broadcasted_iota(jnp.int32, scores.shape, 0)
                column = lax.broadcasted_iota(jnp.int32, scores.shape, 1)
                scores = jnp.where(column <= row, scores, -jnp.inf)
            new_max = jnp.maximum(old_max, jnp.max(scores, -1, keepdims=True))
            weights = jnp.exp2((scores - new_max) * factor).astype(jnp.bfloat16)
            product = jnp.dot(
                weights, v_ref[head, pl.ds(start, width), :], preferred_element_type=jnp.float32
            )
            result.append((new_max, acc * jnp.exp2((old_max - new_max) * factor) + product))
        return tuple(result)

    carry = tuple(
        (jnp.full((rows, 1), floor_value, jnp.float32), jnp.zeros((rows, LANES), jnp.float32))
        for _ in range(heads)
    )
    carry = attend(carry, pl.multiple_of(index * rows, rows), rows, True)
    carry = lax.fori_loop(
        0, index, lambda i, c: attend(c, pl.multiple_of(i * rows, rows), rows, False), carry
    )

    def remote(source, c):
        start = lax.bitwise_xor(own, source) * row_count
        return attend(c, pl.multiple_of(start, row_count), row_count, False)

    carry = lax.fori_loop(0, own, remote, carry)
    outs = [acc[:, NOPE : NOPE + VDIM] / acc[:, :1] for _, acc in carry]
    out_ref[...] = jnp.concatenate(outs, -1).astype(jnp.bfloat16)


def flash(own_index, q_normed, wq, cosine, sine, local, mine, theirs, w_keyval):
    heads = w_keyval.shape[1] // (NOPE + VDIM)
    others = len(mine)
    row_count, packed = local.shape
    tile = min(256, row_count)
    total = row_count * (others + 1)
    scale = float(NOPE + ROPE_DIM) ** (-0.5)

    def whole(array):
        return pl.BlockSpec(array.shape, lambda i, s: (0, 0))

    def tiled(array):
        return pl.BlockSpec((tile, array.shape[1]), lambda i, s: (i, 0))

    operands = (q_normed, wq, cosine, sine, local, *mine, *theirs, w_keyval)
    return pl.pallas_call(
        lambda *refs: attention_kernel(heads, others, scale, *refs),
        out_shape=jax.ShapeDtypeStruct((row_count, heads * VDIM), jnp.bfloat16),
        grid_spec=pltpu.PrefetchScalarGridSpec(
            num_scalar_prefetch=1,
            grid=(row_count // tile,),
            in_specs=[tiled(q_normed), whole(wq), tiled(cosine), tiled(sine)]
            + [whole(x) for x in operands[4:]],
            out_specs=pl.BlockSpec((tile, heads * VDIM), lambda i, s: (i, 0)),
            scratch_shapes=[
                pltpu.VMEM((heads, total, LANES), jnp.bfloat16),
                pltpu.VMEM((heads, total, LANES), jnp.bfloat16),
            ],
        ),
        cost_estimate=pl.CostEstimate(
            flops=4 * heads * row_count * total * LANES,
            bytes_accessed=4 * total * packed,
            transcendentals=heads * row_count * total,
        ),
        compiler_params=pltpu.CompilerParams(vmem_limit_bytes=40 * 1024 * 1024),
        name="attend",
    )(own_index.astype(jnp.int32).reshape(1), *operands)


def expert_kernel(count, steps, with_addend, *refs):
    pieces = refs[:count]
    gate_ref, up_ref, down_ref = refs[count : count + 3]
    rest = refs[count + 3 :]
    if with_addend:
        addend_ref, rest = rest[0], rest[1:]
    outs, (x_ref, total_ref) = rest[:-2], rest[-2:]
    step = pl.program_id(0)
    block = pieces[0].shape[0]

    @pl.when(step == 0)
    def _():
        for i in range(count):
            x_ref[i * block : (i + 1) * block, :] = pieces[i][...]

    inputs = x_ref[...]
    hidden = jnp.dot(inputs, gate_ref[...], preferred_element_type=jnp.float32)
    hidden = hidden / (1.0 + jnp.exp(-hidden))
    hidden = hidden * jnp.dot(inputs, up_ref[...], preferred_element_type=jnp.float32)
    product = jnp.dot(
        hidden.astype(jnp.bfloat16), down_ref[...], preferred_element_type=jnp.float32
    )

    @pl.when(step == 0)
    def _():
        total_ref[...] = product

    @pl.when(step > 0)
    def _():
        total_ref[...] += product

    @pl.when(step == steps - 1)
    def _():
        size = outs[0].shape[0]
        for i, out in enumerate(outs):
            value = total_ref[i * size : (i + 1) * size, :]
            if with_addend:
                value = value.astype(jnp.bfloat16).astype(jnp.float32)
                value = value + addend_ref[i * size : (i + 1) * size, :].astype(jnp.float32)
            out[...] = value.astype(jnp.bfloat16)


def expert_call(pieces, gate, up, down, addend):
    count = len(pieces)
    block, width = pieces[0].shape
    rows = count * block
    hidden = gate.shape[1]
    tile = min(256, hidden)
    steps = hidden // tile
    split = addend is not None
    outs = count if split else 1
    full = lambda shape: pl.BlockSpec(shape, lambda i: (0, 0))
    operands = (*pieces, gate, up, down) + ((addend,) if split else ())
    result = pl.pallas_call(
        lambda *refs: expert_kernel(count, steps, split, *refs),
        out_shape=[jax.ShapeDtypeStruct((rows // outs, width), jnp.bfloat16)] * outs,
        grid=(steps,),
        in_specs=[full((block, width))] * count
        + [
            pl.BlockSpec((width, tile), lambda i: (0, i)),
            pl.BlockSpec((width, tile), lambda i: (0, i)),
            pl.BlockSpec((tile, width), lambda i: (i, 0)),
        ]
        + ([full((rows, width))] if split else []),
        out_specs=[full((rows // outs, width))] * outs,
        scratch_shapes=[
            pltpu.VMEM((rows, width), jnp.bfloat16),
            pltpu.VMEM((rows, width), jnp.float32),
        ],
        cost_estimate=pl.CostEstimate(
            flops=6 * rows * width * hidden,
            bytes_accessed=6 * width * hidden + 4 * rows * width,
            transcendentals=rows * hidden,
        ),
        compiler_params=pltpu.CompilerParams(vmem_limit_bytes=60 * 1024 * 1024),
        name="experts_sum" if split else "experts",
    )(*operands)
    return result if split else result[0]


def dense_body(
    q_latent,
    kv_latent,
    rope_key,
    q_gain,
    kv_gain,
    w_query,
    w_keyval,
    w_output,
    moe_input,
    moe_gain,
    routes,
    route_weight,
    expert_gate,
    expert_up,
    expert_down,
    shared_gate,
    shared_up,
    shared_down,
):
    row_count = q_latent.shape[0]
    half = row_count // 2
    own = lax.axis_index("ep")
    ep_count = lax.axis_size("ep")
    tp_count = lax.axis_size("tp")
    tp_index = lax.axis_index("tp")
    core = tp_index % 2
    depth = tp_index // 2
    depth_count = tp_count // 2
    width = moe_input.shape[1]
    heads_local = w_query.shape[1] // (NOPE + ROPE_DIM)
    halfway = ROPE_DIM // 2
    positions = own * row_count + jnp.arange(row_count, dtype=jnp.int32)
    inverse = rotary_base ** (-(jnp.arange(halfway, dtype=jnp.float32) * 2.0 / ROPE_DIM))
    spread = jnp.concatenate(
        [
            jnp.zeros((NOPE,), jnp.float32),
            inverse,
            inverse,
            jnp.zeros((LANES - NOPE - ROPE_DIM,), jnp.float32),
        ]
    )
    angles = positions.astype(jnp.float32)[:, None] * spread[None, :]
    lane = jnp.arange(LANES)
    cosine = jnp.cos(angles)
    sine = jnp.sin(angles) * jnp.where(lane < NOPE + halfway, -1.0, 1.0)[None, :]

    def exchange(index):
        rope = (index >= NOPE) & (index < NOPE + ROPE_DIM)
        return np.where(rope, NOPE + (index - NOPE + halfway) % ROPE_DIM, -1)

    lanes = np.arange(LANES)
    straight = np.where(lanes < NOPE + ROPE_DIM, lanes, -1)
    swapped = exchange(lanes)
    one_head = np.arange(NOPE + ROPE_DIM)
    pick_straight = np.kron(np.eye(heads_local), one_head[:, None] == straight[None, :])
    pick_swapped = np.kron(np.eye(heads_local), one_head[:, None] == swapped[None, :])
    pick_query = jnp.asarray(np.concatenate([pick_straight, pick_swapped], 1), jnp.bfloat16)
    rope_lane = np.arange(NOPE, NOPE + ROPE_DIM)
    pick_key = jnp.asarray(rope_lane[:, None] == straight[None, :], jnp.bfloat16)
    pick_key_swapped = jnp.asarray(rope_lane[:, None] == swapped[None, :], jnp.bfloat16)

    kv_normed = rms_scale(kv_latent, kv_gain)
    key_rotated = (
        jnp.dot(rope_key, pick_key, preferred_element_type=jnp.float32) * cosine
        + jnp.dot(rope_key, pick_key_swapped, preferred_element_type=jnp.float32) * sine
    ).astype(jnp.bfloat16)
    local_pack = jnp.concatenate([kv_normed, key_rotated], 1)
    sent_pack = lax.dynamic_slice_in_dim(local_pack, core * half, half, 0)
    packs_mine = [move(sent_pack, k, 0) for k in range(1, ep_count)]
    packs_other = [move(pack, 0, 1) for pack in packs_mine]

    grouped = moe_input.reshape(depth_count, 2, MOE_DEV, width)
    own_rows = layer_scale(
        lax.dynamic_index_in_dim(grouped, core, 1, keepdims=False).reshape(-1, width), moe_gain
    )
    other_rows = layer_scale(
        lax.dynamic_index_in_dim(grouped, 1 - core, 1, keepdims=False).reshape(-1, width), moe_gain
    )
    block_rows = own_rows.shape[0]
    arrived = [move(own_rows, k, 0) for k in range(1, ep_count)]

    q_normed = rms_scale(q_latent, q_gain)
    spread_query = jnp.dot(w_query, pick_query, preferred_element_type=jnp.float32).astype(
        jnp.bfloat16
    )
    heads_out = flash(
        own, q_normed, spread_query, cosine, sine, local_pack, packs_mine, packs_other, w_keyval
    )
    arrived, _ = lax.optimization_barrier((arrived, heads_out))
    swapped_rows = [move(piece, 0, 1) for piece in arrived]

    head_parts = [heads_out] + [move(heads_out, 0, 2 * k) for k in range(1, depth_count)]
    heads_mine = jnp.concatenate(head_parts, 1)
    heads_other = move(heads_mine, 0, 1)
    head_rows = heads_local * VDIM

    def output_rows(side):
        return jnp.concatenate(
            [
                lax.dynamic_slice_in_dim(
                    w_output, (2 * jnp.bitwise_xor(depth, k) + side) * head_rows, head_rows, 0
                )
                for k in range(depth_count)
            ],
            0,
        )

    mixed = (
        jnp.dot(heads_mine, output_rows(core), preferred_element_type=jnp.float32)
        + jnp.dot(heads_other, output_rows(1 - core), preferred_element_type=jnp.float32)
    ).astype(jnp.bfloat16)

    def gated(inputs, gate, up, down):
        hidden = jax.nn.silu(jnp.dot(inputs, gate, preferred_element_type=jnp.float32))
        hidden = (hidden * jnp.dot(inputs, up, preferred_element_type=jnp.float32)).astype(
            jnp.bfloat16
        )
        return jnp.dot(hidden, down, preferred_element_type=jnp.float32).astype(jnp.bfloat16)

    shared_both = gated(
        jnp.concatenate([own_rows, other_rows], 0), shared_gate, shared_up, shared_down
    )
    shared_swapped = move(shared_both[block_rows:], 0, 1)
    weights = (expert_gate[0], expert_up[0], expert_down[0])
    routed_other = expert_call([other_rows] + swapped_rows, *weights, None)
    routed_swapped = move(routed_other, 0, 1)
    pair_sum = expert_call([own_rows] + arrived, *weights, routed_swapped)
    returned = [pair_sum[0]] + [move(pair_sum[k], k, 0) for k in range(1, ep_count)]
    own_routes = lax.dynamic_index_in_dim(
        routes.reshape(depth_count, 2, MOE_DEV, -1), core, 1, keepdims=False
    ).reshape(block_rows, -1)
    own_weight = lax.dynamic_index_in_dim(
        route_weight.reshape(depth_count, 2, MOE_DEV, -1), core, 1, keepdims=False
    ).reshape(block_rows, -1)
    summed = shared_both[:block_rows].astype(jnp.float32) + shared_swapped.astype(jnp.float32)
    for k in range(ep_count):
        weight = jnp.sum(
            jnp.where(own_routes == jnp.bitwise_xor(own, k), own_weight, 0.0), -1, keepdims=True
        )
        summed = summed + weight * returned[k].astype(jnp.float32)
    summed = summed.astype(jnp.bfloat16).reshape(depth_count, MOE_DEV, width)
    moe_out = lax.dynamic_index_in_dim(summed, depth, 0, keepdims=False).astype(jnp.float32)
    for k in range(1, depth_count):
        part = lax.dynamic_index_in_dim(summed, jnp.bitwise_xor(depth, k), 0, keepdims=False)
        moe_out = moe_out + move(part, 0, 2 * k).astype(jnp.float32)
    return (mixed, moe_out.astype(jnp.bfloat16))


def solution(mesh):
    in_specs = (
        P("ep", None),
        P("ep", None),
        P("ep", None),
        P(),
        P(),
        P(None, "tp"),
        P(None, "tp"),
        P(None, "tp"),
        P("ep", None),
        P(),
        P("ep", None),
        P("ep", None),
        P("ep", None, "tp"),
        P("ep", None, "tp"),
        P("ep", "tp", None),
        P(None, "tp"),
        P(None, "tp"),
        P("tp", None),
    )
    out_specs = (P("ep", "tp"), P(("ep", "tp"), None))
    if mesh.shape["ep"] > 4:
        return jax.shard_map(
            body, mesh=mesh, in_specs=in_specs, out_specs=out_specs, check_vma=False
        )

    return jax.shard_map(
        dense_body, mesh=mesh, in_specs=in_specs, out_specs=out_specs, check_vma=False
    )
```
